32 devices in a mesh: grp: 2 (over y), dp: 2 (over x), kv: 4 (over z), tp: 2 (over core).
Axes of the slice: x: 2, y: 2, z: 4, core: 2. Of those that a mesh axis runs over, the one named last changes fastest.
Arguments:
- tokens: bfloat16 [4, 1536, 2048], P(('grp', 'dp'), 'kv'), parts along dimension 0, may hold values from -14 to 14
- query_weight: bfloat16 [2048, 1024], P('kv', 'tp'), may hold values from -0.1875 to 0.1875
- key_weight: bfloat16 [2048, 512], P('kv', 'tp'), may hold values from -0.1875 to 0.1875
- value_weight: bfloat16 [2048, 512], P('kv', 'tp'), may hold values from -0.125 to 0.125
- output_weight: bfloat16 [1024, 2048], P('tp', 'kv'), may hold values from -3.59375 to 3.59375
- block_choice: int32 [4, 24, 16], P(('grp', 'dp'), 'kv'), parts along dimension 0, may hold values from -1 to 23, as said below
Outputs:
- attention: bfloat16 [4, 1536, 2048], P(('grp', 'dp'), 'kv', 'tp'), parts along dimension 0
The draws below stay inside these ranges and needn't reach their ends.
There are 2 independent parts, one for each index of `grp`. The reference program is written for one: setup_inputs(seed, part) draws one part's arguments, and reference() takes and returns one part's arrays. A program takes and returns all parts, laid end to end along the dimension named above; an argument that names none is the same for every part. Nothing has to cross between parts.
Inputs may be any that keep to these rules, and one draw needn't show every extreme that they name: `block_choice`: row i of a sequence names distinct key blocks below i, the named ones first and -1 in the slots after them. Split the rows into aligned groups of 6 (the query blocks that share one index of kv, whose key blocks are the same 6 blocks): the rows of one group name at most 4 distinct blocks among those of any other group, and every row of a group names all of exactly 4 blocks of the group just before it.
All inputs are finite; a program needn't handle non-finite values.
Results may differ from the reference program's by a relative error of at most 0.012.
Values may be sent and summed in bfloat16 or wider, within the bound.
A program may use at most 64 MiB of HBM per device.

```python
import jax
import jax.numpy as jnp
from jax import lax

D = 2048
HEADS = 8
KV_HEADS = 4
HEAD = 128
BLOCK = 64
NSEL = 16
CAP = 4
SEQS = 2
LENGTH = 1536
NBLK = 24
QBLK = 6
PARTIALS = 2


def weights_pair(key):
    query_key, noise_key = jax.random.split(jax.random.fold_in(key, 71))
    query_part = jnp.clip(jax.random.normal(query_key, (D, HEADS * HEAD), jnp.float32) * D ** (-0.5), -0.1875, 0.1875)
    noise_part = jnp.clip(jax.random.normal(noise_key, (D, KV_HEADS * HEAD), jnp.float32) * D ** (-0.5), -0.1875, 0.1875)
    return (query_part, noise_part)


def draw_query_weight(key, part):
    query_part, noise_part = weights_pair(key)
    return query_part.astype(jnp.bfloat16)


def draw_key_weight(key, part):
    query_part, noise_part = weights_pair(key)
    return noise_part.astype(jnp.bfloat16)


def draw_tokens(key, part):
    base_key, scale_key = jax.random.split(jax.random.fold_in(key, 13))
    base = jax.random.normal(base_key, (SEQS, LENGTH, D), jnp.float32)
    return jnp.clip(base, -14.0, 14.0).astype(jnp.bfloat16)


def draw_block_choice(key, part):
    owners = NBLK // QBLK
    popular_key, noise_key, priority_key = jax.random.split(jax.random.fold_in(key, 29), 3)
    local_iota = jnp.arange(QBLK, dtype=jnp.int32)
    owner_iota = jnp.arange(owners, dtype=jnp.int32)
    popular = jax.random.randint(popular_key, (SEQS, 1, owners, QBLK), 0, 3) * 4096
    noise_draw = jax.random.randint(noise_key, (SEQS, owners, owners, QBLK), 0, 4096)
    ranking = (noise_draw + popular) * QBLK + local_iota
    chosen_local = lax.top_k(ranking, CAP)[1].astype(jnp.int32)
    remote_ids = (owner_iota[None, None, :, None] * QBLK + chosen_local).reshape(SEQS, owners, owners * CAP)
    remote_owner = jnp.repeat(owner_iota, CAP)
    remote_slot = jnp.tile(jnp.arange(CAP, dtype=jnp.int32), owners)
    requester = owner_iota[:, None]
    remote_valid = remote_owner[None, :] < requester
    forced = (remote_owner[None, :] == requester - 1) | (remote_owner[None, :] == requester - owners // 2) & (remote_slot[None, :] == 0)
    local_ids = requester * QBLK + local_iota[None, :]
    candidates = owners * CAP + QBLK
    id_grid = jnp.concatenate([jnp.broadcast_to(remote_ids[:, :, None, :], (SEQS, owners, QBLK, owners * CAP)), jnp.broadcast_to(local_ids[None, :, None, :], (SEQS, owners, QBLK, QBLK))], axis=3)
    local_valid = jnp.broadcast_to(local_iota[None, None, :] < local_iota[None, :, None], (owners, QBLK, QBLK))
    valid_grid = jnp.concatenate([jnp.broadcast_to(remote_valid[:, None, :], (owners, QBLK, owners * CAP)), local_valid], axis=2)
    forced_grid = jnp.concatenate([jnp.broadcast_to(forced[:, None, :], (owners, QBLK, owners * CAP)), jnp.zeros((owners, QBLK, QBLK), bool)], axis=2)
    priority = jax.random.randint(priority_key, (SEQS, owners, QBLK, candidates), 0, 65536)
    column_iota = jnp.arange(candidates, dtype=jnp.int32)
    ranked = jnp.where(valid_grid, (forced_grid.astype(jnp.int32) * 131072 + priority + 1) * candidates + column_iota, -1 - column_iota)
    best_score, best_index = lax.top_k(ranked, NSEL)
    picked = jnp.take_along_axis(id_grid, best_index.astype(jnp.int32), axis=3)
    result = jnp.where(best_score >= 0, picked, -1)
    return result.reshape(SEQS, NBLK, NSEL).astype(jnp.int32)


def steps_of(own_key, dims, pieces, least, top_value):
    level, own = 1.0, jax.random.fold_in(own_key, 6)
    for axis_at, blocks in pieces:
        heights = jnp.exp(jax.random.uniform(jax.random.fold_in(own, axis_at), (blocks,), jnp.float32, least / len(pieces), top_value / len(pieces)))
        level = level * jnp.repeat(heights, dims[axis_at] // blocks).reshape([-1 if axis == axis_at else 1 for axis in range(len(dims))])
    return level


def scatter_about(own_key, extent, spread, reach, cuts=(), kind=jnp.bfloat16):
    values = jax.random.normal(own_key, extent, jnp.float32) * spread
    if len(cuts) > 0:
        values = steps_of(own_key, extent, cuts, -0.22, 0.18) * values
    return jnp.clip(values, min=-reach, max=reach).astype(kind)


def setup_inputs(seed: int = 0, part: int = 0) -> dict:
    arg_keys = jax.random.split(jax.random.key(seed), 7)
    own_keys = jax.random.split(jax.random.fold_in(arg_keys[6], part), 7)
    tokens = draw_tokens(jax.random.fold_in(jax.random.fold_in(arg_keys[6], part), 71), part)
    query_weight = draw_query_weight(jax.random.fold_in(arg_keys[6], 71), part)
    key_weight = draw_key_weight(jax.random.fold_in(arg_keys[6], 71), part)
    value_weight = scatter_about(arg_keys[3], (D, KV_HEADS * HEAD), D ** -0.5, 0.125, ((0, 4), (1, 2)))
    output_weight = scatter_about(arg_keys[4], (HEADS * HEAD, D), 0.6, 3.59375, ((0, 2), (1, 4)))
    block_choice = draw_block_choice(jax.random.fold_in(jax.random.fold_in(arg_keys[6], part), 71), part)
    return dict(tokens=tokens, query_weight=query_weight, key_weight=key_weight, value_weight=value_weight, output_weight=output_weight, block_choice=block_choice)


THETA = 10000.0
NEGATIVE = -1e30


def rotate(field_rows, positions):
    half_width = HEAD // 2
    inverse = THETA ** (-jnp.arange(half_width, dtype=jnp.float32) / half_width)
    angles = positions.astype(jnp.float32)[:, None] * inverse[None, :]
    cosine = jnp.cos(angles)[:, None, :]
    sine_rows = jnp.sin(angles)[:, None, :]
    first_half = field_rows[..., :half_width]
    second = field_rows[..., half_width:]
    return jnp.concatenate([first_half * cosine - second * sine_rows, second * cosine + first_half * sine_rows], axis=-1)


def one_sequence(features, choice_rows, query_weight, key_weight, value_weight, output_weight):
    positions = jnp.arange(LENGTH, dtype=jnp.int32)
    group_size = HEADS // KV_HEADS
    query_full = jnp.dot(features, query_weight, preferred_element_type=jnp.float32).reshape(LENGTH, HEADS, HEAD)
    queries = lax.optimization_barrier(rotate(query_full, positions).astype(jnp.bfloat16))
    key_full = jnp.dot(features, key_weight, preferred_element_type=jnp.float32).reshape(LENGTH, KV_HEADS, HEAD)
    key_rows = lax.optimization_barrier(rotate(key_full, positions).astype(jnp.bfloat16))
    value_rows = lax.optimization_barrier(jnp.dot(features, value_weight, preferred_element_type=jnp.float32).astype(jnp.bfloat16))
    query_blocks = queries.reshape(NBLK, BLOCK, KV_HEADS, group_size, HEAD)
    key_blocks = key_rows.reshape(NBLK, BLOCK, KV_HEADS, HEAD)
    value_blocks = value_rows.reshape(NBLK, BLOCK, KV_HEADS, HEAD)
    offsets = jnp.arange(BLOCK, dtype=jnp.int32)
    causal = offsets[None, :] <= offsets[:, None]

    def attend(block_index):
        chosen_row = choice_rows[block_index]
        listed = chosen_row >= 0
        picked = jnp.maximum(chosen_row, 0)
        near_keys = jnp.concatenate([key_blocks[picked].reshape(NSEL * BLOCK, KV_HEADS, HEAD), key_blocks[block_index]], axis=0)
        near_values = jnp.concatenate([value_blocks[picked].reshape(NSEL * BLOCK, KV_HEADS, HEAD), value_blocks[block_index]], axis=0)
        listed_keys = jnp.broadcast_to(jnp.repeat(listed, BLOCK)[None, :], (BLOCK, NSEL * BLOCK))
        visible = jnp.concatenate([listed_keys, causal], axis=1)
        scores = jnp.einsum("qgrd,kgd->grqk", query_blocks[block_index].astype(jnp.float32), near_keys.astype(jnp.float32)) * HEAD ** -0.5
        scores = jnp.where(visible[None, None], scores, NEGATIVE)
        row_top = jnp.max(scores, axis=-1, keepdims=True)
        weights = jnp.exp(scores - row_top)
        row_total = jnp.sum(weights, axis=-1)
        rounded = lax.optimization_barrier(weights.astype(jnp.bfloat16))
        weighted = jnp.einsum("grqk,kgd->qgrd", rounded.astype(jnp.float32), near_values.astype(jnp.float32))
        weighted = weighted / jnp.transpose(row_total, (2, 0, 1))[..., None]
        return weighted.astype(jnp.bfloat16)

    mixed = lax.map(attend, jnp.arange(NBLK, dtype=jnp.int32)).reshape(LENGTH, HEADS * HEAD)
    part_width = HEADS * HEAD // PARTIALS
    summed = jnp.zeros((LENGTH, D), jnp.float32)
    for part_index in range(PARTIALS):
        columns = mixed[:, part_index * part_width:(part_index + 1) * part_width]
        piece_out = jnp.dot(columns, output_weight[part_index * part_width:(part_index + 1) * part_width], preferred_element_type=jnp.float32)
        summed = summed + lax.optimization_barrier(piece_out.astype(jnp.bfloat16)).astype(jnp.float32)
    return summed.astype(jnp.bfloat16)


def reference(tokens, query_weight, key_weight, value_weight, output_weight, block_choice):
    def per_sequence(inputs):
        return one_sequence(inputs[0], inputs[1], query_weight, key_weight, value_weight, output_weight)

    return lax.map(per_sequence, (tokens, block_choice))
```

```python
import functools

import jax
import jax.numpy as jnp
from jax import lax
from jax.experimental import pallas as pl
from jax.experimental.pallas import tpu as pltpu
from jax.sharding import PartitionSpec as P

HEAD = 128
BLOCK = 64
THETA = 10000.0
NEGATIVE = -1e30
MESH = pl.DeviceIdType.MESH
QUARTERS = 4


def kernel(n, tokens_hbm, wk_hbm, wv_hbm, wq_hbm, wo_hbm, cos_ref, sin_ref, bias_ref, out_ref,
           tokens, wk_all, wv_all, wq_all, wo_all, kpool, vpool, qbuf, mixed, outgoing, incoming,
           own_sem, z_send, z_recv, xy_send, xy_recv, kv_send, kv_recv, tp_send, tp_recv):
    g, d, z, t = (lax.axis_index(a) for a in ("grp", "dp", "kv", "tp"))
    gx, dx, tx = g + 1 - 2 * (g % 2), d + 1 - 2 * (d % 2), 1 - t
    up, down = jnp.minimum(z + 1, n - 1), jnp.maximum(z - 1, 0)
    up_id, down_id, tp_id = (g, d, up, t), (g, d, down, t), (g, d, z, tx)
    plane = ((g, dx, z, t), (gx, d, z, t), (gx, dx, z, t))
    mine = (g % 2) * 2 + d % 2
    theirs = ((g % 2) * 2 + dx % 2, (gx % 2) * 2 + d % 2, (gx % 2) * 2 + dx % 2)
    rows = tokens.shape[0]
    shards = (wk_hbm, wv_hbm, wq_hbm, wo_hbm)
    gathered = (wk_all, wv_all, wq_all, wo_all)
    depths = tuple(s.shape[0] for s in shards)
    parts = tuple(x // QUARTERS for x in depths)

    def place(w, origin, quarter):
        start = pl.multiple_of(quarter * parts[w], parts[w])
        return gathered[w].at[origin, pl.ds(start, parts[w])]

    def own_copy(w):
        return pltpu.make_async_copy(shards[w], gathered[w].at[z], own_sem.at[w])

    tokens_copy = pltpu.make_async_copy(tokens_hbm, tokens, own_sem.at[4])

    def z_copy(w, origin, way, own=False):
        start = pl.multiple_of(mine * parts[w], parts[w])
        source = shards[w].at[pl.ds(start, parts[w])] if own else place(w, origin, mine)
        return pltpu.make_async_remote_copy(
            src_ref=source, dst_ref=place(w, origin, mine),
            send_sem=z_send.at[w, origin, way], recv_sem=z_recv.at[w, origin],
            device_id=(up_id, down_id)[way], device_id_type=MESH)

    def xy_copy(w, origin, peer, arriving=False):
        where = place(w, origin, theirs[peer] if arriving else mine)
        return pltpu.make_async_remote_copy(
            src_ref=where, dst_ref=where,
            send_sem=xy_send.at[w, origin, peer], recv_sem=xy_recv.at[w, origin, peer],
            device_id=plane[peer], device_id_type=MESH)

    def kv_copy(which, origin):
        pool = (kpool, vpool)[which]
        where = pool.at[pl.ds(pl.multiple_of(origin * rows, rows), rows)]
        return pltpu.make_async_remote_copy(
            src_ref=where, dst_ref=where, send_sem=kv_send.at[which, origin],
            recv_sem=kv_recv.at[which, origin], device_id=up_id, device_id_type=MESH)

    def tp_copy(j):
        return pltpu.make_async_remote_copy(
            src_ref=outgoing.at[j], dst_ref=incoming.at[j], send_sem=tp_send.at[j],
            recv_sem=tp_recv.at[j], device_id=tp_id, device_id_type=MESH)

    def send_own(w):
        @pl.when(z + 1 < n)
        def _():
            z_copy(w, z, 0, True).start()

        @pl.when(z > 0)
        def _():
            z_copy(w, z, 1, True).start()

    def relay(w):
        def step(s, carry):
            @pl.when(z - s >= 0)
            def _():
                origin = z - s
                z_copy(w, origin, 0).wait_recv()
                for peer in range(3):
                    xy_copy(w, origin, peer).start()

                @pl.when(z + 1 < n)
                def _():
                    z_copy(w, origin, 0).start()

            @pl.when(z + s < n)
            def _():
                origin = z + s
                z_copy(w, origin, 1).wait_recv()
                for peer in range(3):
                    xy_copy(w, origin, peer).start()

                @pl.when(z > 0)
                def _():
                    z_copy(w, origin, 1).start()
            return carry
        lax.fori_loop(1, n, step, 0)

    def settle(w):
        own_copy(w).wait()

        def step(s, carry):
            origin = (z + s) % n
            for peer in range(3):
                xy_copy(w, origin, peer, True).wait_recv()
            return carry
        lax.fori_loop(1, n, step, 0)

    def kv_relay(first, last):
        def step(s, carry):
            @pl.when(z - s >= 0)
            def _():
                for which in range(2):
                    kv_copy(which, z - s).wait_recv()

                    @pl.when(z + 1 < n)
                    def _():
                        kv_copy(which, z - s).start()
            return carry
        lax.fori_loop(first, last, step, 0)

    tokens_copy.start()
    for w in range(4):
        own_copy(w).start()

    barrier = pltpu.get_barrier_semaphore()
    for peer in plane + (tp_id,):
        pl.semaphore_signal(barrier, inc=1, device_id=peer, device_id_type=MESH)

    @pl.when(z + 1 < n)
    def _():
        pl.semaphore_signal(barrier, inc=1, device_id=up_id, device_id_type=MESH)

    @pl.when(z > 0)
    def _():
        pl.semaphore_signal(barrier, inc=1, device_id=down_id, device_id_type=MESH)
    pl.semaphore_wait(barrier, 4 + jnp.where(z + 1 < n, 1, 0) + jnp.where(z > 0, 1, 0))

    def project(gathered_ref):
        total = None
        depth = gathered_ref.shape[1]
        for origin in range(n):
            piece = jnp.dot(tokens[:, origin * depth:(origin + 1) * depth], gathered_ref[origin],
                            preferred_element_type=jnp.float32)
            total = piece if total is None else total + piece
        return total

    def turned(total):
        heads = total.shape[1] // HEAD
        out = []
        for h in range(heads):
            u = total[:, h * HEAD:(h + 1) * HEAD]
            out.append(u * cos_ref[...] + pltpu.roll(u, HEAD // 2, 1) * sin_ref[...])
        return jnp.concatenate(out, axis=1).astype(jnp.bfloat16)

    send_own(0)
    send_own(1)
    relay(0)
    send_own(2)
    relay(1)
    send_own(3)
    relay(2)
    tokens_copy.wait()
    here = pl.ds(pl.multiple_of(z * rows, rows), rows)
    def clear(s, carry):
        @pl.when(z + s < n)
        def _():
            past = pl.ds(pl.multiple_of((z + s) * rows, rows), rows)
            kpool[past] = jnp.zeros((rows, kpool.shape[1]), kpool.dtype)
            vpool[past] = jnp.zeros((rows, vpool.shape[1]), vpool.dtype)
        return carry
    lax.fori_loop(1, n, clear, 0)
    settle(0)
    kpool[here] = turned(project(wk_all))
    settle(1)
    vpool[here] = project(wv_all).astype(jnp.bfloat16)

    @pl.when(z + 1 < n)
    def _():
        kv_copy(0, z).start()
        kv_copy(1, z).start()
    relay(3)
    kv_relay(1, min(2, n))
    settle(2)
    qbuf[...] = turned(project(wq_all))
    kv_relay(min(2, n), n)

    kv_heads = kpool.shape[1] // HEAD
    group = qbuf.shape[1] // kpool.shape[1]
    contract = (((1,), (1,)), ((), ()))

    def attend(i, carry):
        at = pl.multiple_of(i * BLOCK, BLOCK)
        near = pl.multiple_of(z * rows + i * BLOCK, BLOCK)
        bias = bias_ref[i]
        row = lax.broadcasted_iota(jnp.int32, (group * BLOCK, BLOCK), 0) % BLOCK
        column = lax.broadcasted_iota(jnp.int32, (group * BLOCK, BLOCK), 1)
        for h in range(kv_heads):
            lanes = slice(h * HEAD, (h + 1) * HEAD)
            q = jnp.concatenate([
                qbuf[pl.ds(at, BLOCK), (h * group + r) * HEAD:(h * group + r + 1) * HEAD]
                for r in range(group)], axis=0)
            far = lax.dot_general(q, kpool[:, lanes], contract,
                                  preferred_element_type=jnp.float32) * HEAD ** (-0.5) + bias
            own = lax.dot_general(q, kpool[pl.ds(near, BLOCK), lanes], contract,
                                  preferred_element_type=jnp.float32) * HEAD ** (-0.5)
            own = jnp.where(column <= row, own, NEGATIVE)
            top = jnp.maximum(jnp.max(far, axis=1, keepdims=True), jnp.max(own, axis=1, keepdims=True))
            far = jnp.exp(far - top)
            own = jnp.exp(own - top)
            total = jnp.sum(far, axis=1, keepdims=True) + jnp.sum(own, axis=1, keepdims=True)
            weighted = jnp.dot(far.astype(jnp.bfloat16), vpool[:, lanes],
                               preferred_element_type=jnp.float32)
            weighted += jnp.dot(own.astype(jnp.bfloat16), vpool[pl.ds(near, BLOCK), lanes],
                                preferred_element_type=jnp.float32)
            weighted = (weighted / total).astype(jnp.bfloat16)
            for r in range(group):
                mixed[pl.ds(at, BLOCK), (h * group + r) * HEAD:(h * group + r + 1) * HEAD] = (
                    weighted[r * BLOCK:(r + 1) * BLOCK])
        return carry
    lax.fori_loop(0, rows // BLOCK, attend, 0)

    settle(3)
    half = n // 2
    width = wo_all.shape[2]
    for j in range(half):
        outgoing[j] = jnp.dot(mixed[...], wo_all[tx * half + j],
                              preferred_element_type=jnp.float32).astype(jnp.bfloat16)
        if j > 0:
            tp_copy(j - 1).start()
    for j in range(half):
        out_ref[:, j * width:(j + 1) * width] = jnp.dot(
            mixed[...], wo_all[t * half + j], preferred_element_type=jnp.float32).astype(jnp.bfloat16)
        if j == 0:
            tp_copy(half - 1).start()
    for j in range(half):
        tp_copy(j).wait_recv()
        columns = slice(j * width, (j + 1) * width)
        out_ref[:, columns] = (out_ref[:, columns].astype(jnp.float32)
                               + incoming[j].astype(jnp.float32)).astype(jnp.bfloat16)

    for j in range(half):
        tp_copy(j).wait_send()

    def drain(origin, carry):
        @pl.when(origin <= z)
        def _():
            @pl.when(z + 1 < n)
            def _():
                for which in range(2):
                    kv_copy(which, origin).wait_send()
                for w in range(4):
                    z_copy(w, origin, 0).wait_send()

        @pl.when(origin >= z)
        def _():
            @pl.when(z > 0)
            def _():
                for w in range(4):
                    z_copy(w, origin, 1).wait_send()

        @pl.when(origin != z)
        def _():
            for w in range(4):
                for peer in range(3):
                    xy_copy(w, origin, peer).wait_send()
        return carry
    lax.fori_loop(0, n, drain, 0)


def on_device(n, tokens, query_weight, key_weight, value_weight, output_weight, block_choice):
    features = tokens[0]
    rows, model = features.shape
    z = lax.axis_index("kv")
    query_width = query_weight.shape[1]
    key_width = key_weight.shape[1]
    blocks = rows // BLOCK
    keys = n * rows
    half_width = HEAD // 2
    positions = z * rows + jnp.arange(rows, dtype=jnp.int32)
    inverse = THETA ** (-jnp.arange(half_width, dtype=jnp.float32) / half_width)
    angles = positions.astype(jnp.float32)[:, None] * inverse[None, :]
    cosine, sine = jnp.cos(angles), jnp.sin(angles)
    cosine = jnp.concatenate([cosine, cosine], axis=1)
    sine = jnp.concatenate([-sine, sine], axis=1)
    named = jnp.any(block_choice[0][:, :, None] == jnp.arange(keys // BLOCK, dtype=jnp.int32), axis=1)
    bias = jnp.repeat(jnp.where(named, 0.0, NEGATIVE).astype(jnp.float32), BLOCK, axis=1)
    bias = bias[:, None, :]
    anywhere = pl.BlockSpec(memory_space=pl.ANY)
    inside = pl.BlockSpec(memory_space=pltpu.VMEM)
    depth = key_weight.shape[0]
    out_rows, out_columns = output_weight.shape
    bf16 = jnp.bfloat16
    dma = pltpu.SemaphoreType.DMA
    out = pl.pallas_call(
        functools.partial(kernel, n),
        out_shape=jax.ShapeDtypeStruct((rows, n * out_columns // 2), bf16),
        in_specs=[anywhere] * 5 + [inside] * 3,
        out_specs=inside,
        scratch_shapes=[
            pltpu.VMEM((rows, model), bf16),
            pltpu.VMEM((n, depth, key_width), bf16),
            pltpu.VMEM((n, depth, key_width), bf16),
            pltpu.VMEM((n, depth, query_width), bf16),
            pltpu.VMEM((n, out_rows, out_columns), bf16),
            pltpu.VMEM((keys, key_width), bf16),
            pltpu.VMEM((keys, key_width), bf16),
            pltpu.VMEM((rows, query_width), bf16),
            pltpu.VMEM((rows, query_width), bf16),
            pltpu.VMEM((n // 2, rows, out_columns), bf16),
            pltpu.VMEM((n // 2, rows, out_columns), bf16),
            dma((5,)), dma((4, n, 2)), dma((4, n)), dma((4, n, 3)), dma((4, n, 3)),
            dma((2, n)), dma((2, n)), dma((n // 2,)), dma((n // 2,)),
        ],
        compiler_params=pltpu.CompilerParams(
            collective_id=0, has_side_effects=True, vmem_limit_bytes=60 * 1024 * 1024),
    )(features, key_weight, value_weight, query_weight, output_weight, cosine, sine, bias)
    return out[None]


def solution(mesh):
    return jax.shard_map(
        functools.partial(on_device, mesh.shape["kv"]),
        mesh=mesh,
        in_specs=(
            P(("grp", "dp"), "kv", None),
            P("kv", "tp"),
            P("kv", "tp"),
            P("kv", "tp"),
            P("tp", "kv"),
            P(("grp", "dp"), "kv", None),
        ),
        out_specs=P(("grp", "dp"), "kv", "tp"),
        check_vma=False,
    )
```

```python
import functools

import jax
import numpy as np
import jax.numpy as jnp
from jax import lax
from jax.experimental import pallas as pl
from jax.experimental.pallas import tpu as pltpu
from jax.sharding import PartitionSpec as P

HEAD = 128
BLOCK = 64
THETA = 10000.0
NEGATIVE = -1e30
MESH = pl.DeviceIdType.MESH
QUARTERS = 4


def kernel(n, tokens_hbm, wk_hbm, wv_hbm, wq_hbm, wo_hbm, choice_ref, frequency_ref, out_ref,
           tokens, wk_all, wv_all, wq_all, wo_all, kpool, vpool, qbuf, mixed, outgoing, incoming, kept, cosine, sine,
           own_sem, z_send, z_recv, xy_send, xy_recv, kv_send, kv_recv, tp_send, tp_recv):
    g, d, z, t = (lax.axis_index(a) for a in ("grp", "dp", "kv", "tp"))
    gx, dx, tx = g + 1 - 2 * (g % 2), d + 1 - 2 * (d % 2), 1 - t
    up, down = jnp.minimum(z + 1, n - 1), jnp.maximum(z - 1, 0)
    up_id, down_id, tp_id = (g, d, up, t), (g, d, down, t), (g, d, z, tx)
    plane = ((g, dx, z, t), (gx, d, z, t), (gx, dx, z, t))
    mine = (g % 2) * 2 + d % 2
    theirs = ((g % 2) * 2 + dx % 2, (gx % 2) * 2 + d % 2, (gx % 2) * 2 + dx % 2)
    rows = tokens.shape[0]
    half = n // 2
    shards = (wk_hbm, wv_hbm, wq_hbm, wo_hbm)
    gathered = (wk_all, wv_all, wq_all, wo_all)
    depths = tuple(s.shape[0] for s in shards)
    parts = tuple(x // QUARTERS for x in depths)

    def place(w, origin, quarter):
        start = pl.multiple_of(quarter * parts[w], parts[w])
        return gathered[w].at[origin, pl.ds(start, parts[w])]

    def own_copy(w):
        return pltpu.make_async_copy(shards[w], gathered[w].at[z], own_sem.at[w])

    tokens_copy = pltpu.make_async_copy(tokens_hbm.at[0], tokens, own_sem.at[4])

    def z_copy(w, origin, way, own=False):
        start = pl.multiple_of(mine * parts[w], parts[w])
        source = shards[w].at[pl.ds(start, parts[w])] if own else place(w, origin, mine)
        return pltpu.make_async_remote_copy(
            src_ref=source, dst_ref=place(w, origin, mine),
            send_sem=z_send.at[w, origin, way], recv_sem=z_recv.at[w, origin],
            device_id=(up_id, down_id)[way], device_id_type=MESH)

    def xy_copy(w, origin, peer, arriving=False):
        where = place(w, origin, theirs[peer] if arriving else mine)
        return pltpu.make_async_remote_copy(
            src_ref=where, dst_ref=where,
            send_sem=xy_send.at[w, origin, peer], recv_sem=xy_recv.at[w, origin, peer],
            device_id=plane[peer], device_id_type=MESH)

    def kv_copy(which, origin):
        pool = (kpool, vpool)[which]
        where = pool.at[pl.ds(pl.multiple_of(origin * rows, rows), rows)]
        return pltpu.make_async_remote_copy(
            src_ref=where, dst_ref=where, send_sem=kv_send.at[which, origin],
            recv_sem=kv_recv.at[which, origin], device_id=up_id, device_id_type=MESH)

    def tp_copy(j):
        return pltpu.make_async_remote_copy(
            src_ref=outgoing.at[j], dst_ref=incoming.at[j], send_sem=tp_send.at[j],
            recv_sem=tp_recv.at[j], device_id=tp_id, device_id_type=MESH)

    def send_own(w):
        @pl.when(z + 1 < n)
        def _():
            z_copy(w, z, 0, True).start()

        @pl.when(z > 0)
        def _():
            z_copy(w, z, 1, True).start()

    def relay(w, first=1, last=n):
        def step(s, carry):
            @pl.when(z - s >= 0)
            def _():
                origin = z - s
                z_copy(w, origin, 0).wait_recv()
                for peer in range(3):
                    xy_copy(w, origin, peer).start()

                @pl.when(z + 1 < n)
                def _():
                    z_copy(w, origin, 0).start()

            @pl.when(z + s < n)
            def _():
                origin = z + s
                z_copy(w, origin, 1).wait_recv()
                for peer in range(3):
                    xy_copy(w, origin, peer).start()

                @pl.when(z > 0)
                def _():
                    z_copy(w, origin, 1).start()
            return carry
        lax.fori_loop(first, last, step, 0)

    def settle(w):
        own_copy(w).wait()

        def step(s, carry):
            origin = (z + s) % n
            for peer in range(3):
                xy_copy(w, origin, peer, True).wait_recv()
            return carry
        lax.fori_loop(1, n, step, 0)

    def kv_relay(first, last):
        def step(s, carry):
            @pl.when(z - s >= 0)
            def _():
                for which in range(2):
                    kv_copy(which, z - s).wait_recv()

                    @pl.when(z + 1 < n)
                    def _():
                        kv_copy(which, z - s).start()
            return carry
        lax.fori_loop(first, last, step, 0)

    tokens_copy.start()
    for w in range(4):
        own_copy(w).start()

    barrier = pltpu.get_barrier_semaphore()
    for peer in plane + (tp_id,):
        pl.semaphore_signal(barrier, inc=1, device_id=peer, device_id_type=MESH)

    @pl.when(z + 1 < n)
    def _():
        pl.semaphore_signal(barrier, inc=1, device_id=up_id, device_id_type=MESH)

    @pl.when(z > 0)
    def _():
        pl.semaphore_signal(barrier, inc=1, device_id=down_id, device_id_type=MESH)
    pl.semaphore_wait(barrier, 4 + jnp.where(z + 1 < n, 1, 0) + jnp.where(z > 0, 1, 0))

    def project(gathered_ref):
        total = None
        depth = gathered_ref.shape[1]
        for origin in range(n):
            piece = jnp.dot(tokens[:, origin * depth:(origin + 1) * depth], gathered_ref[origin],
                            preferred_element_type=jnp.float32)
            total = piece if total is None else total + piece
        return total

    def turned(total):
        heads = total.shape[1] // HEAD
        out = []
        for h in range(heads):
            u = total[:, h * HEAD:(h + 1) * HEAD]
            out.append(u * cosine[...] + pltpu.roll(u, HEAD // 2, 1) * sine[...])
        return jnp.concatenate(out, axis=1).astype(jnp.bfloat16)

    send_own(0)
    send_own(1)
    spot = z * rows + lax.broadcasted_iota(jnp.int32, cosine.shape, 0)
    angle = spot.astype(jnp.float32) * frequency_ref[...]
    lane = lax.broadcasted_iota(jnp.int32, cosine.shape, 1)
    cosine[...] = jnp.cos(angle)
    sine[...] = jnp.sin(angle) * jnp.where(lane < HEAD // 2, -1.0, 1.0)
    relay(0)
    send_own(2)
    relay(1)
    send_own(3)
    relay(2)
    relay(3, 1, half)
    tokens_copy.wait()
    here = pl.ds(pl.multiple_of(z * rows, rows), rows)
    def clear(s, carry):
        @pl.when(z + s < n)
        def _():
            past = pl.ds(pl.multiple_of((z + s) * rows, rows), rows)
            kpool[past] = jnp.zeros((rows, kpool.shape[1]), kpool.dtype)
            vpool[past] = jnp.zeros((rows, vpool.shape[1]), vpool.dtype)
        return carry
    lax.fori_loop(1, n, clear, 0)
    settle(0)
    kpool[here] = turned(project(wk_all))
    settle(1)
    vpool[here] = project(wv_all).astype(jnp.bfloat16)

    @pl.when(z + 1 < n)
    def _():
        kv_copy(0, z).start()
        kv_copy(1, z).start()
    relay(3, half, n)
    kv_relay(1, min(2, n))
    settle(2)
    qbuf[...] = turned(project(wq_all))
    kv_relay(min(2, n), n)

    kv_heads = kpool.shape[1] // HEAD
    group = qbuf.shape[1] // kpool.shape[1]
    contract = (((1,), (1,)), ((), ()))

    def attend(i, carry):
        at = pl.multiple_of(i * BLOCK, BLOCK)
        near = pl.multiple_of(z * rows + i * BLOCK, BLOCK)
        named = None
        block = lax.broadcasted_iota(jnp.int32, (1, kpool.shape[0]), 1) // BLOCK
        for slot in range(choice_ref.shape[2]):
            match = block == choice_ref[0, i, slot]
            named = match if named is None else named | match
        bias = jnp.where(named, 0.0, NEGATIVE)
        row = lax.broadcasted_iota(jnp.int32, (group * BLOCK, BLOCK), 0) % BLOCK
        column = lax.broadcasted_iota(jnp.int32, (group * BLOCK, BLOCK), 1)
        for h in range(kv_heads):
            lanes = slice(h * HEAD, (h + 1) * HEAD)
            q = jnp.concatenate([
                qbuf[pl.ds(at, BLOCK), (h * group + r) * HEAD:(h * group + r + 1) * HEAD]
                for r in range(group)], axis=0)
            far = lax.dot_general(q, kpool[:, lanes], contract,
                                  preferred_element_type=jnp.float32) * HEAD ** (-0.5) + bias
            own = lax.dot_general(q, kpool[pl.ds(near, BLOCK), lanes], contract,
                                  preferred_element_type=jnp.float32) * HEAD ** (-0.5)
            own = jnp.where(column <= row, own, NEGATIVE)
            top = jnp.maximum(jnp.max(far, axis=1, keepdims=True), jnp.max(own, axis=1, keepdims=True))
            far = jnp.exp(far - top)
            own = jnp.exp(own - top)
            total = jnp.sum(far, axis=1, keepdims=True) + jnp.sum(own, axis=1, keepdims=True)
            weighted = jnp.dot(far.astype(jnp.bfloat16), vpool[:, lanes],
                               preferred_element_type=jnp.float32)
            weighted += jnp.dot(own.astype(jnp.bfloat16), vpool[pl.ds(near, BLOCK), lanes],
                                preferred_element_type=jnp.float32)
            weighted = (weighted / total).astype(jnp.bfloat16)
            for r in range(group):
                mixed[pl.ds(at, BLOCK), (h * group + r) * HEAD:(h * group + r + 1) * HEAD] = (
                    weighted[r * BLOCK:(r + 1) * BLOCK])
        return carry
    lax.fori_loop(0, rows // BLOCK, attend, 0)

    own_copy(3).wait()
    width = wo_all.shape[2]

    def finish(origin):
        piece = jnp.dot(mixed[...], wo_all[origin],
                        preferred_element_type=jnp.float32).astype(jnp.bfloat16)
        slot = origin % half

        @pl.when(origin // half == tx)
        def _():
            outgoing[slot] = piece
            tp_copy(slot).start()

        @pl.when(origin // half == t)
        def _():
            kept[slot] = piece

    finish(z)

    def collect(s, carry):
        for origin, there in ((z - s, z - s >= 0), (z + s, z + s < n)):
            @pl.when(there)
            def _():
                for peer in range(3):
                    xy_copy(3, origin, peer, True).wait_recv()
                finish(origin)
        return carry
    lax.fori_loop(1, n, collect, 0)
    for j in range(half):
        tp_copy(j).wait_recv()
        columns = slice(j * width, (j + 1) * width)
        out_ref[0, :, columns] = (kept[j].astype(jnp.float32)
                                  + incoming[j].astype(jnp.float32)).astype(jnp.bfloat16)

    for j in range(half):
        tp_copy(j).wait_send()

    def drain(origin, carry):
        @pl.when(origin <= z)
        def _():
            @pl.when(z + 1 < n)
            def _():
                for which in range(2):
                    kv_copy(which, origin).wait_send()
                for w in range(4):
                    z_copy(w, origin, 0).wait_send()

        @pl.when(origin >= z)
        def _():
            @pl.when(z > 0)
            def _():
                for w in range(4):
                    z_copy(w, origin, 1).wait_send()

        @pl.when(origin != z)
        def _():
            for w in range(4):
                for peer in range(3):
                    xy_copy(w, origin, peer).wait_send()
        return carry
    lax.fori_loop(0, n, drain, 0)


def on_device(n, tokens, query_weight, key_weight, value_weight, output_weight, block_choice):
    rows, model = tokens.shape[1:]
    query_width = query_weight.shape[1]
    key_width = key_weight.shape[1]
    keys = n * rows
    half_width = HEAD // 2
    inverse = (THETA ** (-np.arange(half_width) / half_width)).astype(np.float32)
    frequency = np.concatenate([inverse, inverse])[None]
    anywhere = pl.BlockSpec(memory_space=pl.ANY)
    inside = pl.BlockSpec(memory_space=pltpu.VMEM)
    depth = key_weight.shape[0]
    out_rows, out_columns = output_weight.shape
    bf16 = jnp.bfloat16
    dma = pltpu.SemaphoreType.DMA
    out = pl.pallas_call(
        functools.partial(kernel, n),
        out_shape=jax.ShapeDtypeStruct((1, rows, n * out_columns // 2), bf16),
        in_specs=[anywhere] * 5 + [pl.BlockSpec(memory_space=pltpu.SMEM), inside],
        out_specs=inside,
        scratch_shapes=[
            pltpu.VMEM((rows, model), bf16),
            pltpu.VMEM((n, depth, key_width), bf16),
            pltpu.VMEM((n, depth, key_width), bf16),
            pltpu.VMEM((n, depth, query_width), bf16),
            pltpu.VMEM((n, out_rows, out_columns), bf16),
            pltpu.VMEM((keys, key_width), bf16),
            pltpu.VMEM((keys, key_width), bf16),
            pltpu.VMEM((rows, query_width), bf16),
            pltpu.VMEM((rows, query_width), bf16),
            pltpu.VMEM((n // 2, rows, out_columns), bf16),
            pltpu.VMEM((n // 2, rows, out_columns), bf16),
            pltpu.VMEM((n // 2, rows, out_columns), bf16),
            pltpu.VMEM((rows, HEAD), jnp.float32),
            pltpu.VMEM((rows, HEAD), jnp.float32),
            dma((5,)), dma((4, n, 2)), dma((4, n)), dma((4, n, 3)), dma((4, n, 3)),
            dma((2, n)), dma((2, n)), dma((n // 2,)), dma((n // 2,)),
        ],
        compiler_params=pltpu.CompilerParams(
            collective_id=0, has_side_effects=True, vmem_limit_bytes=60 * 1024 * 1024),
    )(tokens, key_weight, value_weight, query_weight, output_weight, block_choice, frequency)
    return out


def solution(mesh):
    return jax.shard_map(
        functools.partial(on_device, mesh.shape["kv"]),
        mesh=mesh,
        in_specs=(
            P(("grp", "dp"), "kv", None),
            P("kv", "tp"),
            P("kv", "tp"),
            P("kv", "tp"),
            P("tp", "kv"),
            P(("grp", "dp"), "kv", None),
        ),
        out_specs=P(("grp", "dp"), "kv", "tp"),
        check_vma=False,
    )
```
